256 devices in a mesh: grp: 2 (over y), sp: 32 (over z, core), tp: 4 (over x).
Axes of the slice: x: 4, y: 2, z: 16, core: 2. Of those that a mesh axis runs over, the one named last changes fastest.
The devices are a block of a 4x16x16 slice.
Arguments:
- residual_in: bfloat16 [20480, 2048], P(('grp', 'sp', 'tp')), parts along dimension 0, may hold values from -6 to 6
- narrow_query_rows: bfloat16 [20480, 1024], P(('grp', 'sp'), 'tp'), parts along dimension 0, may hold values from -5 to 5
- wide_query_rows: bfloat16 [20480, 1024], P(('grp', 'sp'), 'tp'), parts along dimension 0, may hold values from -5 to 5
- narrow_key_value: bfloat16 [20480, 4, 128], P(('grp', 'sp'), 'tp'), parts along dimension 0, may hold values from -120 to 120
- wide_key_value: bfloat16 [20480, 4, 256], P(('grp', 'sp'), 'tp'), parts along dimension 0, may hold values from -120 to 120
- narrow_norm_gains: float32 [2, 64], replicated, may hold values from 0.1 to 10
- wide_norm_gains: float32 [2, 128], replicated, may hold values from 0.1 to 10
- out_narrow: bfloat16 [1024, 2048], P('tp'), may hold values from -0.1875 to 0.1875
- out_wide: bfloat16 [1024, 2048], P('tp'), may hold values from -0.1875 to 0.1875
- mixer_gain: float32 [2048], replicated, may hold values from 0.1 to 1.9
- mixer_gate: bfloat16 [2048, 5632], P('sp', 'tp'), may hold values from -0.125 to 0.125
- mixer_up: bfloat16 [2048, 5632], P('sp', 'tp'), may hold values from -0.125 to 0.125
- mixer_down: bfloat16 [5632, 2048], P('tp', 'sp'), may hold values from -0.078125 to 0.078125
Outputs:
- layer_out: bfloat16 [20480, 2048], P(('grp', 'sp', 'tp')), parts along dimension 0
The draws below stay inside these ranges and needn't reach their ends.
There are 2 independent parts, one for each index of `grp`. The reference program is written for one: setup_inputs(seed, part) draws one part's arguments, and reference() takes and returns one part's arrays. A program takes and returns all parts, laid end to end along the dimension named above; an argument that names none is the same for every part. Nothing has to cross between parts.
All inputs are finite; a program needn't handle non-finite values.
Results may differ from the reference program's by a relative error of at most 0.015.
The reference program's roundings to bfloat16 on the way count: a program that leaves them out, or rounds other values in their place, can miss the bound.
Values may be sent and summed in bfloat16 or wider, within the bound.
No kernel may reach another device: no remote copies, remote signals or barrier semaphores. Data moves between devices by JAX's collectives and lax.ppermute only.
A program may use at most 128 MiB of HBM per device.

```python
import math
import jax
import jax.numpy as jnp
from jax import lax

D = 2048
FF = 5632
NARROW_HEAD_SIZE = 64
WIDE_HEAD_SIZE = 128
NARROW_QUERIES = 16
NARROW_KEY_HEADS = 4
WIDE_QUERIES = 8
WIDE_KEY_HEADS = 4
GRID = 64
TOKENS = 10240
N_TP = 4


def plain_entries(key, shape):
    return jnp.clip(jax.random.normal(key, shape, jnp.float32), -5.0, 5.0)


def value_entries(key, shape):
    return jnp.clip(24.0 * jax.random.normal(key, shape, jnp.float32), -120.0, 120.0)


def group_keys(key, heads, width, salt):
    return plain_entries(jax.random.fold_in(key, salt), (TOKENS, heads, width))


def group_query_heads(key, heads, key_heads, width, salt):
    queries = plain_entries(jax.random.fold_in(key, salt + 1), (TOKENS, heads, width))
    return queries.reshape(TOKENS, heads * width)


def group_key_value(key, heads, width, salt):
    keys = group_keys(key, heads, width, salt)
    values = value_entries(jax.random.fold_in(key, salt + 2), (TOKENS, heads, width))
    return jnp.concatenate([keys, values], axis=-1)


def group_gains(key, width, salt):
    inner = jax.random.fold_in(key, salt)
    return jnp.clip(1.0 + 0.18 * jax.random.normal(inner, (2, width), jnp.float32), 0.1, 1.9)


def draw_narrow_query_rows(key, part):
    return group_query_heads(key, NARROW_QUERIES, NARROW_KEY_HEADS, NARROW_HEAD_SIZE, 100).astype(jnp.bfloat16)


def draw_wide_query_rows(key, part):
    return group_query_heads(key, WIDE_QUERIES, WIDE_KEY_HEADS, WIDE_HEAD_SIZE, 200).astype(jnp.bfloat16)


def draw_narrow_key_value(key, part):
    return group_key_value(key, NARROW_KEY_HEADS, NARROW_HEAD_SIZE, 100).astype(jnp.bfloat16)


def draw_wide_key_value(key, part):
    return group_key_value(key, WIDE_KEY_HEADS, WIDE_HEAD_SIZE, 200).astype(jnp.bfloat16)


def draw_narrow_norm_gains(key, part):
    return group_gains(key, NARROW_HEAD_SIZE, 300)


def draw_wide_norm_gains(key, part):
    return group_gains(key, WIDE_HEAD_SIZE, 400)


def level_of(stream_key, dims, split, low, top_value):
    def one(dim, blocks):
        heights = jax.random.uniform(jax.random.fold_in(jax.random.fold_in(stream_key, 6), dim), (blocks,), jnp.float32, low / len(split), top_value / len(split))
        return jnp.repeat(jnp.exp(heights), dims[dim] // blocks).reshape((-1,) + (1,) * (len(dims) - dim - 1))

    factor_of = one(*split[0])
    for cut in split[1:]:
        factor_of = factor_of * one(*cut)
    return factor_of


def scatter_about(key, extent, scale, bound, shards=(), kind=jnp.bfloat16):
    entries = scale * jax.random.normal(key, extent, jnp.float32)
    if shards:
        entries = entries * level_of(key, extent, shards, -0.22, 0.18)
    return jnp.clip(entries, -bound, bound).astype(kind)


def setup_inputs(seed: int = 0, part: int = 0) -> dict:
    key_list = jax.random.split(jax.random.key(seed), 14)
    own_keys = jax.random.split(jax.random.fold_in(key_list[13], part), 14)
    residual_in = scatter_about(own_keys[0], (TOKENS, D), 1.0, 6.0, ((0, 128),))
    narrow_query_rows = draw_narrow_query_rows(jax.random.fold_in(jax.random.fold_in(key_list[13], part), 71), part)
    wide_query_rows = draw_wide_query_rows(jax.random.fold_in(jax.random.fold_in(key_list[13], part), 71), part)
    narrow_key_value = draw_narrow_key_value(jax.random.fold_in(jax.random.fold_in(key_list[13], part), 71), part)
    wide_key_value = draw_wide_key_value(jax.random.fold_in(jax.random.fold_in(key_list[13], part), 71), part)
    narrow_norm_gains = draw_narrow_norm_gains(jax.random.fold_in(key_list[13], 71), part)
    wide_norm_gains = draw_wide_norm_gains(jax.random.fold_in(key_list[13], 71), part)
    out_narrow = scatter_about(key_list[7], (NARROW_QUERIES * NARROW_HEAD_SIZE, D), (NARROW_QUERIES * NARROW_HEAD_SIZE) ** -0.5, 0.1875, ((0, 4),))
    out_wide = scatter_about(key_list[8], (WIDE_QUERIES * WIDE_HEAD_SIZE, D), (WIDE_QUERIES * WIDE_HEAD_SIZE) ** -0.5, 0.1875, ((0, 4),))
    mixer_gain = jnp.clip(1.0 + 0.18 * jax.random.normal(key_list[9], (D,), jnp.float32), 0.1, 1.9)
    mixer_gate = scatter_about(key_list[10], (D, FF), D ** -0.5, 0.125, ((0, 32), (1, 4)))
    mixer_up = scatter_about(key_list[11], (D, FF), D ** -0.5, 0.125, ((0, 32), (1, 4)))
    mixer_down = scatter_about(key_list[12], (FF, D), FF ** -0.5, 0.078125, ((0, 4), (1, 32)))
    return {"residual_in": residual_in, "narrow_query_rows": narrow_query_rows, "wide_query_rows": wide_query_rows, "narrow_key_value": narrow_key_value, "wide_key_value": wide_key_value, "narrow_norm_gains": narrow_norm_gains, "wide_norm_gains": wide_norm_gains, "out_narrow": out_narrow, "out_wide": out_wide, "mixer_gain": mixer_gain, "mixer_gate": mixer_gate, "mixer_up": mixer_up, "mixer_down": mixer_down}


eps = 1e-06
theta = 10000.0

def rounded(value):
    return lax.optimization_barrier(value.astype(jnp.bfloat16)).astype(jnp.float32)

def grid_angles(width):
    positions = jnp.arange(TOKENS, dtype=jnp.int32)
    quarter = width // 4
    freqs = theta ** (-jnp.arange(quarter, dtype=jnp.float32) * 4.0 / width)
    row = (positions // GRID).astype(jnp.float32)
    column = (positions % GRID).astype(jnp.float32)
    return jnp.concatenate([row[:, None] * freqs[None, :], column[:, None] * freqs[None, :]], axis=-1)

def prepare(raw, gain, angles):
    field = raw.astype(jnp.float32)
    field = field * lax.rsqrt(lax.optimization_barrier(jnp.mean(field * field, axis=-1, keepdims=True)) + eps) * gain.astype(jnp.float32)
    half = field.shape[-1] // 2
    cosine = jnp.cos(angles)[:, None, :]
    sine = jnp.sin(angles)[:, None, :]
    first = field[..., :half]
    second = field[..., half:]
    turned = jnp.concatenate([first * cosine - second * sine, second * cosine + first * sine], axis=-1)
    return rounded(turned)

def attend_heads(query_raw, keyval, gains, heads, key_heads, width):
    angles = grid_angles(width)
    queries = prepare(query_raw.reshape(TOKENS, heads, width), gains[0], angles)
    keys = prepare(keyval[:, :, :width], gains[1], angles)
    values = keyval[:, :, width:].astype(jnp.float32)
    group = heads // key_heads
    block = math.gcd(TOKENS, 128)
    blocks = queries.reshape(TOKENS // block, block, key_heads, group, width)

    def one(piece):
        scores = jnp.einsum('qkgd,skd->kgqs', piece, keys) / math.sqrt(width)
        peak = lax.optimization_barrier(jnp.max(scores, axis=-1, keepdims=True))
        weights = jnp.exp(scores - peak)
        total = lax.optimization_barrier(jnp.sum(weights, axis=-1))
        summed = jnp.einsum('kgqs,skd->qkgd', rounded(weights), values)
        return (summed / jnp.transpose(total, (2, 0, 1))[..., None]).astype(jnp.bfloat16)
    result = lax.map(one, blocks)
    return result.reshape(TOKENS, heads * width)

def reference(residual_in, narrow_query_rows, wide_query_rows, narrow_key_value, wide_key_value, narrow_norm_gains, wide_norm_gains, out_narrow, out_wide, mixer_gain, mixer_gate, mixer_up, mixer_down):
    attention_narrow = attend_heads(narrow_query_rows, narrow_key_value, narrow_norm_gains, NARROW_QUERIES, NARROW_KEY_HEADS, NARROW_HEAD_SIZE)
    attention_wide = attend_heads(wide_query_rows, wide_key_value, wide_norm_gains, WIDE_QUERIES, WIDE_KEY_HEADS, WIDE_HEAD_SIZE)
    cols_narrow = NARROW_QUERIES * NARROW_HEAD_SIZE // N_TP
    cols_wide = WIDE_QUERIES * WIDE_HEAD_SIZE // N_TP
    attended = jnp.zeros((TOKENS, D), jnp.float32)
    for index in range(N_TP):
        lo_n = index * cols_narrow
        lo_w = index * cols_wide
        part = jnp.dot(attention_narrow[:, lo_n:lo_n + cols_narrow], out_narrow[lo_n:lo_n + cols_narrow], preferred_element_type=jnp.float32)
        part = part + jnp.dot(attention_wide[:, lo_w:lo_w + cols_wide], out_wide[lo_w:lo_w + cols_wide], preferred_element_type=jnp.float32)
        attended = attended + rounded(part)
    attended = attended.astype(jnp.bfloat16)
    stream = residual_in.astype(jnp.float32) + attended.astype(jnp.float32)
    scale = lax.rsqrt(lax.optimization_barrier(jnp.mean(stream * stream, axis=-1, keepdims=True)) + eps)
    normed = (stream * scale * mixer_gain.astype(jnp.float32)).astype(jnp.bfloat16)
    gate = jnp.dot(normed, mixer_gate, preferred_element_type=jnp.float32)
    up = jnp.dot(normed, mixer_up, preferred_element_type=jnp.float32)
    hidden = (jax.nn.silu(gate) * up).astype(jnp.bfloat16)
    units = FF // N_TP
    branch = jnp.zeros((TOKENS, D), jnp.float32)
    for index in range(N_TP):
        lo_u = index * units
        branch = branch + rounded(jnp.dot(hidden[:, lo_u:lo_u + units], mixer_down[lo_u:lo_u + units], preferred_element_type=jnp.float32))
    branch = branch.astype(jnp.bfloat16)
    return (stream + branch.astype(jnp.float32)).astype(jnp.bfloat16)
```

```python
import functools
import math

import jax
import jax.numpy as jnp
from jax import lax
from jax.experimental import pallas as pl
from jax.experimental.pallas import tpu as pltpu
from jax.sharding import PartitionSpec as P


GRID = 64
LANES = 128
LOG2E = math.log2(math.e)

eps = 1e-06
theta = 10000.0


def grid_angles(positions, width):
    quarter = width // 4
    freqs = theta ** (-jnp.arange(quarter, dtype=jnp.float32) * 4.0 / width)
    row = (positions // GRID).astype(jnp.float32)
    column = (positions % GRID).astype(jnp.float32)
    return jnp.concatenate(
        [row[:, None] * freqs[None, :], column[:, None] * freqs[None, :]], axis=-1
    )


def prepare(raw, gain, angles):
    field = raw.astype(jnp.float32)
    field = field * lax.rsqrt(jnp.mean(field * field, axis=-1, keepdims=True) + eps) * gain
    half = field.shape[-1] // 2
    cosine = jnp.cos(angles)[:, None, :]
    sine = jnp.sin(angles)[:, None, :]
    first = field[..., :half]
    second = field[..., half:]
    turned = jnp.concatenate(
        [first * cosine - second * sine, second * cosine + first * sine], axis=-1
    )
    return turned.astype(jnp.bfloat16)


def head_rows(raw, gain, angles, width):
    tokens = raw.shape[0]
    heads = raw.shape[1] // width
    queries = prepare(raw.reshape(tokens, heads, width), gain, angles)
    queries = jnp.transpose(queries, (1, 0, 2)).reshape(heads * tokens, width)
    return jnp.pad(queries, ((0, 0), (0, LANES - width)))


def stage_kernel(*refs, chunks, first, heads, tokens):
    count = len(heads)
    q_refs = refs[:2]
    kv_refs = refs[2 : 2 + chunks]
    refs = refs[2 + chunks :]
    if first:
        in_refs, out_refs = (None, refs)
    else:
        in_refs, out_refs = (refs[:3], refs[3:])
    stats_out = out_refs[2]
    blocks = [(side, h) for h in range(count) for side in range(2)]

    def scores(side, h):
        key_at, _, scale = heads[h]
        queries = q_refs[side][h * tokens : (h + 1) * tokens, :]
        keys = jnp.concatenate([r[:, key_at : key_at + LANES] for r in kv_refs], axis=0)
        s = lax.dot_general(
            queries, keys, (((1,), (1,)), ((), ())), preferred_element_type=jnp.float32
        )
        return s * scale

    if first:
        stats_out[...] = jnp.zeros(stats_out.shape, jnp.float32)
    ahead = scores(*blocks[0])
    for n, (side, h) in enumerate(blocks):
        s = ahead
        if n + 1 < len(blocks):
            ahead = scores(*blocks[n + 1])
        value_at = heads[h][1]
        rows = slice(h * tokens, (h + 1) * tokens)
        at = side * count + h
        total_at = LANES // 2 + at
        peak = jnp.max(s, axis=-1, keepdims=True)
        if not first:
            old = in_refs[2][:, at : at + 1]
            peak = jnp.maximum(peak, old)
            rescale = jnp.exp2(old - peak)
        weights = jnp.exp2(s - peak)
        total = jnp.sum(weights, axis=-1, keepdims=True)
        values = jnp.concatenate([r[:, value_at : value_at + LANES] for r in kv_refs], axis=0)
        summed = jnp.dot(
            weights.astype(jnp.bfloat16), values, preferred_element_type=jnp.float32
        )
        if not first:
            total = total + rescale * in_refs[2][:, total_at : total_at + 1]
            summed = summed + rescale * in_refs[side][rows, :]
        stats_out[:, at : at + 1] = peak
        stats_out[:, total_at : total_at + 1] = total
        out_refs[side][rows, :] = summed


def stage(queries, pieces, state, heads, tokens):
    rows = queries[0].shape[0]
    keys = sum(p.shape[0] for p in pieces)
    first = state is None
    operands = (*queries, *pieces, *(() if first else state))
    shapes = [
        jax.ShapeDtypeStruct((rows, LANES), jnp.float32),
        jax.ShapeDtypeStruct((rows, LANES), jnp.float32),
        jax.ShapeDtypeStruct((tokens, LANES), jnp.float32),
    ]
    whole = pl.BlockSpec(memory_space=pltpu.VMEM)
    return pl.pallas_call(
        functools.partial(
            stage_kernel, chunks=len(pieces), first=first, heads=heads, tokens=tokens
        ),
        in_specs=[whole] * len(operands),
        out_specs=[whole] * 3,
        out_shape=shapes,
        compiler_params=pltpu.CompilerParams(vmem_limit_bytes=40 << 20),
        cost_estimate=pl.CostEstimate(
            flops=2 * rows * keys * LANES * 4,
            bytes_accessed=keys * 768 + 8 * rows * LANES * 4,
            transcendentals=2 * rows * keys,
        ),
        name="attend_stage",
    )(*operands)


def merge_kernel(own_acc, own_stats, other_acc, other_stats, out_ref, *, heads, widths, tokens):
    count = len(heads)
    column = 0
    held = None
    for h in range(count):
        rows = slice(h * tokens, (h + 1) * tokens)
        here, there = (h, count + h)
        half = LANES // 2
        peak_a = own_stats[:, here : here + 1]
        peak_b = other_stats[:, there : there + 1]
        peak = jnp.maximum(peak_a, peak_b)
        scale_a = jnp.exp2(peak_a - peak)
        scale_b = jnp.exp2(peak_b - peak)
        total = (
            scale_a * own_stats[:, half + here : half + here + 1]
            + scale_b * other_stats[:, half + there : half + there + 1]
        )
        summed = scale_a * own_acc[rows, :] + scale_b * other_acc[rows, :]
        result = summed / total
        if widths[h] == LANES:
            out_ref[:, column : column + LANES] = result.astype(out_ref.dtype)
            column += LANES
        elif held is None:
            held = result[:, half:]
        else:
            pair = jnp.concatenate([held, result[:, half:]], axis=1)
            out_ref[:, column : column + LANES] = pair.astype(out_ref.dtype)
            column += LANES
            held = None


def merge(own, other, heads, widths, tokens):
    columns = sum(widths)
    whole = pl.BlockSpec(memory_space=pltpu.VMEM)
    return pl.pallas_call(
        functools.partial(merge_kernel, heads=heads, widths=widths, tokens=tokens),
        in_specs=[whole] * 4,
        out_specs=whole,
        out_shape=jax.ShapeDtypeStruct((tokens, columns), jnp.bfloat16),
        compiler_params=pltpu.CompilerParams(vmem_limit_bytes=32 << 20),
        cost_estimate=pl.CostEstimate(
            flops=8 * len(heads) * tokens * LANES,
            bytes_accessed=8 * len(heads) * tokens * LANES,
            transcendentals=2 * len(heads) * tokens,
        ),
        name="merge_cores",
    )(*own, *other)


def after(value, *others):
    return lax.optimization_barrier((value, *others))[0]


def layer(
    residual_in,
    narrow_query_rows,
    wide_query_rows,
    narrow_key_value,
    wide_key_value,
    narrow_norm_gains,
    wide_norm_gains,
    out_narrow,
    out_wide,
    mixer_gain,
    mixer_gate,
    mixer_up,
    mixer_down,
):
    n_sp = lax.axis_size("sp")
    n_tp = lax.axis_size("tp")
    sp_at = lax.axis_index("sp")
    tp_at = lax.axis_index("tp")
    chips = n_sp // 2
    up_ring = [(i, (i + 2) % n_sp) for i in range(n_sp)]
    down_ring = [(i, (i - 2) % n_sp) for i in range(n_sp)]
    sibling = [(i, i ^ 1) for i in range(n_sp)]
    right = [(i, (i + 1) % n_tp) for i in range(n_tp)]
    left = [(i, (i - 1) % n_tp) for i in range(n_tp)]

    units = mixer_gate.shape[1]
    mixer_rows = jnp.concatenate([mixer_gate, mixer_up, mixer_down.T], axis=1)
    mixer_whole = lax.all_gather(mixer_rows, "sp", axis=0, tiled=True)

    tokens = narrow_query_rows.shape[0]
    narrow_width = narrow_key_value.shape[2] // 2
    wide_width = wide_key_value.shape[2] // 2
    positions = sp_at * tokens + jnp.arange(tokens, dtype=jnp.int32)
    angles_narrow = grid_angles(positions, narrow_width)
    angles_wide = grid_angles(positions, wide_width)
    narrow_keys = prepare(narrow_key_value[:, :, :narrow_width], narrow_norm_gains[1], angles_narrow)
    wide_keys = prepare(wide_key_value[:, :, :wide_width], wide_norm_gains[1], angles_wide)
    own_piece = jnp.concatenate(
        [
            narrow_keys[:, 0],
            narrow_key_value[:, 0, narrow_width:],
            wide_keys[:, 0],
            wide_key_value[:, 0, wide_width:],
        ],
        axis=1,
    )

    narrow_count = narrow_query_rows.shape[1] // narrow_width
    wide_count = wide_query_rows.shape[1] // wide_width
    heads = [(0, 0, LOG2E / math.sqrt(narrow_width))] * narrow_count
    heads += [(LANES, 2 * LANES, LOG2E / math.sqrt(wide_width))] * wide_count
    widths = [narrow_width] * narrow_count + [wide_width] * wide_count

    hop_up = lax.ppermute(own_piece, "sp", up_ring)
    hop_down = lax.ppermute(own_piece, "sp", down_ring)
    queries = jnp.concatenate(
        [
            head_rows(narrow_query_rows, narrow_norm_gains[0], angles_narrow, narrow_width),
            head_rows(wide_query_rows, wide_norm_gains[0], angles_wide, wide_width),
        ],
        axis=0,
    )
    both = (queries, lax.ppermute(queries, "sp", sibling))

    out_rows = (out_narrow, out_wide)
    out_right = [lax.ppermute(w, "tp", right) for w in out_rows]
    out_left = [lax.ppermute(w, "tp", left) for w in out_rows]
    res_right = lax.ppermute(residual_in, "tp", right)
    res_left = lax.ppermute(residual_in, "tp", left)

    state = None
    pieces = [own_piece]
    for hop in range(1, chips // 2 + 1):
        pieces += [hop_up, hop_down]
        if state is not None:
            hop_up, hop_down, *state = lax.optimization_barrier((hop_up, hop_down, *state))
        if hop + 1 < chips // 2:
            sent_up, sent_down = (hop_up, hop_down)
        elif hop + 1 == chips // 2:
            sent_up, sent_down = (hop_up[: tokens // 2], hop_down[tokens // 2 :])
        if hop < chips // 2:
            hop_up = lax.ppermute(sent_up, "sp", up_ring)
            hop_down = lax.ppermute(sent_down, "sp", down_ring)
        state = stage(both, pieces, state, heads, tokens)
        pieces = []
        if hop == max(chips // 2 - 2, 1):
            half = residual_in.shape[1] // 2
            out_far = (
                lax.ppermute(after(out_right[0], state[2]), "tp", right),
                lax.ppermute(after(out_left[1], state[2]), "tp", left),
            )
            res_far = jnp.concatenate(
                [
                    lax.ppermute(after(res_right, state[2])[:, :half], "tp", right),
                    lax.ppermute(after(res_left, state[2])[:, half:], "tp", left),
                ],
                axis=1,
            )

    other_acc = lax.ppermute(state[1], "sp", sibling)
    other_stats = lax.ppermute(state[2], "sp", sibling)
    attn = merge((state[0], state[2]), (other_acc, other_stats), heads, widths, tokens)

    cut = narrow_count * narrow_width
    attn_right = lax.ppermute(attn, "tp", right)
    attn_left = lax.ppermute(attn, "tp", left)
    attn_far = (
        lax.ppermute(attn_right[:, :cut], "tp", right),
        lax.ppermute(attn_left[:, cut:], "tp", left),
    )

    def projected(narrow, wide, weights):
        total = jnp.dot(narrow, weights[0], preferred_element_type=jnp.float32)
        total = total + jnp.dot(wide, weights[1], preferred_element_type=jnp.float32)
        return total.astype(jnp.bfloat16).astype(jnp.float32)

    def cut_in_two(a):
        return (a[:, :cut], a[:, cut:])

    attended = projected(*cut_in_two(attn), out_rows)
    attended = attended + projected(*cut_in_two(attn_right), out_right)
    attended = attended + projected(*cut_in_two(attn_left), out_left)
    attended = attended + projected(*attn_far, out_far)
    attended = attended.astype(jnp.bfloat16)

    owned = residual_in.shape[0]
    turned = jnp.concatenate([residual_in, res_left, res_far, res_right] * 2, axis=0)
    residual = lax.dynamic_slice_in_dim(turned, (n_tp - tp_at) * owned % tokens, tokens, 0)
    stream = residual.astype(jnp.float32) + attended.astype(jnp.float32)
    scale = lax.rsqrt(jnp.mean(stream * stream, axis=-1, keepdims=True) + eps)
    normed = (stream * scale * mixer_gain).astype(jnp.bfloat16)

    gate = jnp.dot(normed, mixer_whole[:, :units], preferred_element_type=jnp.float32)
    up = jnp.dot(normed, mixer_whole[:, units : 2 * units], preferred_element_type=jnp.float32)
    hidden = (jax.nn.silu(gate) * up).astype(jnp.bfloat16)
    terms = lax.dot_general(
        hidden,
        mixer_whole[:, 2 * units :],
        (((1,), (1,)), ((), ())),
        preferred_element_type=jnp.float32,
    ).astype(jnp.bfloat16)
    parts = lax.all_to_all(terms.reshape(n_tp, owned, -1), "tp", 0, 0, tiled=True)
    branch = jnp.sum(parts.astype(jnp.float32), axis=0).astype(jnp.bfloat16)
    own_stream = residual_in.astype(jnp.float32) + lax.dynamic_slice_in_dim(
        attended, tp_at * owned, owned, 0
    ).astype(jnp.float32)
    return (own_stream + branch.astype(jnp.float32)).astype(jnp.bfloat16)


def solution(mesh):
    placed = (
        P(("grp", "sp", "tp"), None),
        P(("grp", "sp"), "tp"),
        P(("grp", "sp"), "tp"),
        P(("grp", "sp"), "tp", None),
        P(("grp", "sp"), "tp", None),
        P(),
        P(),
        P("tp", None),
        P("tp", None),
        P(),
        P("sp", "tp"),
        P("sp", "tp"),
        P("tp", "sp"),
    )
    return jax.shard_map(
        layer, mesh=mesh, in_specs=placed, out_specs=P(("grp", "sp", "tp"), None), check_vma=False
    )
```

```python
import functools
import math

import jax
import jax.numpy as jnp
from jax import lax
from jax.experimental import pallas as pl
from jax.experimental.pallas import tpu as pltpu
from jax.sharding import PartitionSpec as P


GRID = 64
LANES = 128
LOG2E = math.log2(math.e)

eps = 1e-06
theta = 10000.0


def grid_angles(positions, width):
    quarter = width // 4
    freqs = theta ** (-jnp.arange(quarter, dtype=jnp.float32) * 4.0 / width)
    row = (positions // GRID).astype(jnp.float32)
    column = (positions % GRID).astype(jnp.float32)
    return jnp.concatenate(
        [row[:, None] * freqs[None, :], column[:, None] * freqs[None, :]], axis=-1
    )


def prepare(raw, gain, angles):
    field = raw.astype(jnp.float32)
    field = field * lax.rsqrt(jnp.mean(field * field, axis=-1, keepdims=True) + eps) * gain
    half = field.shape[-1] // 2
    cosine = jnp.cos(angles)[:, None, :]
    sine = jnp.sin(angles)[:, None, :]
    first = field[..., :half]
    second = field[..., half:]
    turned = jnp.concatenate(
        [first * cosine - second * sine, second * cosine + first * sine], axis=-1
    )
    return turned.astype(jnp.bfloat16)


def head_rows(raw, gain, angles, width):
    tokens = raw.shape[0]
    heads = raw.shape[1] // width
    queries = prepare(raw.reshape(tokens, heads, width), gain, angles)
    queries = jnp.transpose(queries, (1, 0, 2)).reshape(heads * tokens, width)
    return jnp.pad(queries, ((0, 0), (0, LANES - width)))


def stage_kernel(*refs, chunks, first, split, count, scales, tokens):
    q_refs = refs[:2]
    kv_refs = refs[2 : 2 + chunks]
    refs = refs[2 + chunks :]
    in_refs, out_refs = (None, refs) if first else (refs[:6], refs[6:])
    keys_here = sum(r.shape[0] for r in kv_refs)
    ones = jnp.ones((keys_here, LANES), jnp.bfloat16)

    def visit(h, carry):
        narrow = h < split
        key_at = pl.multiple_of(jnp.where(narrow, 0, LANES), LANES)
        value_at = pl.multiple_of(jnp.where(narrow, 0, 2 * LANES), LANES)
        scale = jnp.where(narrow, scales[0], scales[1])
        rows = pl.ds(pl.multiple_of(h * tokens, 16), tokens)
        keys = jnp.concatenate([r[:, pl.ds(key_at, LANES)] for r in kv_refs], axis=0)
        values = jnp.concatenate([r[:, pl.ds(value_at, LANES)] for r in kv_refs], axis=0)
        values = jnp.concatenate([values, ones], axis=1)
        scores = [
            lax.dot_general(
                q[rows, :], keys, (((1,), (1,)), ((), ())), preferred_element_type=jnp.float32
            )
            * scale
            for q in q_refs
        ]
        for side in range(2):
            s = scores[side]
            peak = jnp.max(s, axis=-1, keepdims=True)
            peak = jnp.broadcast_to(peak, (tokens, LANES))
            if not first:
                old = in_refs[2 + side][rows, :]
                peak = jnp.maximum(peak, old)
                rescale = jnp.exp2(old - peak)
            weights = jnp.concatenate(
                [
                    jnp.exp2(s[:, at : at + LANES] - peak[:, : min(LANES, keys_here - at)])
                    for at in range(0, keys_here, LANES)
                ],
                axis=1,
            ).astype(jnp.bfloat16)
            both = jnp.dot(weights, values, preferred_element_type=jnp.float32)
            summed = both[:, :LANES]
            total = both[:, LANES:]
            if not first:
                total = total + rescale * in_refs[4 + side][rows, :]
                summed = summed + rescale * in_refs[side][rows, :]
            out_refs[side][rows, :] = summed
            out_refs[2 + side][rows, :] = peak
            out_refs[4 + side][rows, :] = total
        return carry

    lax.fori_loop(0, count, visit, 0)


def stage(queries, pieces, state, split, count, scales, tokens):
    rows = queries[0].shape[0]
    keys = sum(p.shape[0] for p in pieces)
    first = state is None
    operands = (*queries, *pieces, *(() if first else state))
    whole = pl.BlockSpec(memory_space=pltpu.VMEM)
    return pl.pallas_call(
        functools.partial(
            stage_kernel,
            chunks=len(pieces),
            first=first,
            split=split,
            count=count,
            scales=scales,
            tokens=tokens,
        ),
        in_specs=[whole] * len(operands),
        out_specs=[whole] * 6,
        out_shape=[jax.ShapeDtypeStruct((rows, LANES), jnp.float32)] * 6,
        compiler_params=pltpu.CompilerParams(vmem_limit_bytes=32 << 20),
        cost_estimate=pl.CostEstimate(
            flops=2 * rows * keys * LANES * 4,
            bytes_accessed=keys * 768 + 12 * rows * LANES * 4,
            transcendentals=2 * rows * keys,
        ),
        name="attend_stage",
    )(*operands)


def merge_kernel(acc_a, peak_a, total_a, acc_b, peak_b, total_b, out_ref, *, widths, tokens):
    column = 0
    held = None
    half = LANES // 2
    for h in range(len(widths)):
        rows = slice(h * tokens, (h + 1) * tokens)
        high_a = peak_a[rows, :]
        high_b = peak_b[:, h : h + 1]
        peak = jnp.maximum(high_a, high_b)
        scale_a = jnp.exp2(high_a - peak)
        scale_b = jnp.exp2(high_b - peak)
        total = scale_a * total_a[rows, :] + scale_b * total_b[:, h : h + 1]
        summed = scale_a * acc_a[rows, :] + scale_b * acc_b[rows, :]
        result = summed / total
        if widths[h] == LANES:
            out_ref[:, column : column + LANES] = result.astype(out_ref.dtype)
            column += LANES
        elif held is None:
            held = result[:, half:]
        else:
            pair = jnp.concatenate([held, result[:, half:]], axis=1)
            out_ref[:, column : column + LANES] = pair.astype(out_ref.dtype)
            column += LANES
            held = None


def merge(own, other, widths, tokens):
    columns = sum(widths)
    whole = pl.BlockSpec(memory_space=pltpu.VMEM)
    return pl.pallas_call(
        functools.partial(merge_kernel, widths=widths, tokens=tokens),
        in_specs=[whole] * 6,
        out_specs=whole,
        out_shape=jax.ShapeDtypeStruct((tokens, columns), jnp.bfloat16),
        compiler_params=pltpu.CompilerParams(vmem_limit_bytes=32 << 20),
        cost_estimate=pl.CostEstimate(
            flops=8 * len(widths) * tokens * LANES,
            bytes_accessed=16 * len(widths) * tokens * LANES,
            transcendentals=2 * len(widths) * tokens,
        ),
        name="merge_cores",
    )(*own, *other)


def project_kernel(
    at_ref, gain_ref, *refs, split, owned, members
):
    own, right, left, far_narrow, far_wide = refs[:5]
    out_narrow, out_wide, early_right, early_left, early_narrow, early_wide, kept = refs[5:12]
    normed_ref, stream_ref, attended_ref = refs[12:]
    width = attended_ref.shape[1]
    rows = out_narrow.shape[0]
    ends = 2 * rows
    pieces = [
        (own[:, :split], own[:, split:], out_narrow, 0, out_wide, 0),
        (right[:, :split], right[:, split:], early_right, 0, early_right, rows),
        (left[:, :split], left[:, split:], early_left, 0, early_left, rows),
        (far_narrow[...], far_wide[...], early_narrow, 0, early_wide, 0),
    ]
    residuals = [
        kept[...],
        early_left[ends:, :],
        early_wide[rows:, :],
        early_right[ends:, :],
    ]
    block = min(width, 512)
    for at in range(0, width, block):
        columns = slice(at, at + block)
        attended = None
        for narrow, wide, first, first_at, second, second_at in pieces:
            part = jnp.dot(
                narrow,
                first[first_at : first_at + rows, columns],
                preferred_element_type=jnp.float32,
            ) + jnp.dot(
                wide,
                second[second_at : second_at + rows, columns],
                preferred_element_type=jnp.float32,
            )
            part = part.astype(jnp.bfloat16).astype(jnp.float32)
            attended = part if attended is None else attended + part
        attended_ref[:, columns] = attended.astype(jnp.bfloat16).astype(jnp.float32)
    here = at_ref[0]
    for k in range(members):
        start = pl.multiple_of(lax.rem(here + k, members) * owned, 8)
        stream = residuals[k].astype(jnp.float32) + attended_ref[pl.ds(start, owned), :]
        if k == 0:
            stream_ref[...] = stream
        scale = lax.rsqrt(jnp.mean(stream * stream, axis=-1, keepdims=True) + eps)
        normed = stream * scale * gain_ref[...]
        normed_ref[k * owned : (k + 1) * owned, :] = normed.astype(jnp.bfloat16)


def project(at, gain, attn, weights, residual, split):
    owned, width = residual.shape
    rows = attn[0].shape[0]
    operands = (*attn, *weights, residual)
    whole = pl.BlockSpec(memory_space=pltpu.VMEM)
    return pl.pallas_call(
        functools.partial(project_kernel, split=split, owned=owned, members=rows // owned),
        in_specs=[pl.BlockSpec(memory_space=pltpu.SMEM)] + [whole] * (1 + len(operands)),
        out_specs=[whole] * 2,
        out_shape=[
            jax.ShapeDtypeStruct((rows, width), jnp.bfloat16),
            jax.ShapeDtypeStruct((owned, width), jnp.float32),
        ],
        scratch_shapes=[pltpu.VMEM((rows, width), jnp.float32)],
        compiler_params=pltpu.CompilerParams(vmem_limit_bytes=40 << 20),
        cost_estimate=pl.CostEstimate(
            flops=2 * rows * width * 8 * weights[0].shape[0],
            bytes_accessed=16 * width * weights[0].shape[0] + 6 * rows * width,
            transcendentals=rows,
        ),
        name="project",
    )(at.reshape(1), gain.reshape(1, width), *operands)


def mixer_kernel(rows_ref, in_ref, down_ref, *refs):
    out_refs = refs[:-2]
    gate_ref, hidden_ref = refs[-2:]
    step = pl.program_id(0)
    owned = out_refs[0].shape[0]

    @pl.when(step < 2)
    def _():
        product = jnp.dot(rows_ref[...], in_ref[...], preferred_element_type=jnp.float32)

        @pl.when(step == 0)
        def _():
            gate_ref[...] = product

        @pl.when(step == 1)
        def _():
            gate = gate_ref[...]
            hidden = gate / (1.0 + jnp.exp(-gate)) * product
            hidden_ref[...] = hidden.astype(jnp.bfloat16)

    @pl.when(step >= 2)
    def _():
        terms = lax.dot_general(
            hidden_ref[...],
            down_ref[...],
            (((1,), (1,)), ((), ())),
            preferred_element_type=jnp.float32,
        ).astype(jnp.bfloat16)
        for n, out_ref in enumerate(out_refs):
            out_ref[...] = terms[n * owned : (n + 1) * owned, :]


def mix(rows, whole, units, members):
    count, width = rows.shape
    owned = count // members
    depth = min(width, 512)
    return pl.pallas_call(
        mixer_kernel,
        grid=(2 + width // depth,),
        in_specs=[
            pl.BlockSpec((count, width), lambda i: (0, 0)),
            pl.BlockSpec((width, units), lambda i: (0, jnp.minimum(i, 1))),
            pl.BlockSpec((depth, units), lambda i: (jnp.maximum(i - 2, 0), 2)),
        ],
        out_specs=[pl.BlockSpec((owned, depth), lambda i: (0, jnp.maximum(i - 2, 0)))]
        * members,
        out_shape=[jax.ShapeDtypeStruct((owned, width), jnp.bfloat16)] * members,
        scratch_shapes=[
            pltpu.VMEM((count, units), jnp.float32),
            pltpu.VMEM((count, units), jnp.bfloat16),
        ],
        compiler_params=pltpu.CompilerParams(
            vmem_limit_bytes=40 << 20, dimension_semantics=("arbitrary",)
        ),
        cost_estimate=pl.CostEstimate(
            flops=6 * count * width * units,
            bytes_accessed=6 * width * units + 4 * count * width,
            transcendentals=count * units,
        ),
        name="mixer",
    )(rows, whole, whole)


def layer(
    residual_in,
    narrow_query_rows,
    wide_query_rows,
    narrow_key_value,
    wide_key_value,
    narrow_norm_gains,
    wide_norm_gains,
    out_narrow,
    out_wide,
    mixer_gain,
    mixer_gate,
    mixer_up,
    mixer_down,
):
    n_sp = lax.axis_size("sp")
    n_tp = lax.axis_size("tp")
    sp_at = lax.axis_index("sp")
    tp_at = lax.axis_index("tp")
    chips = n_sp // 2
    up_ring = [(i, (i + 2) % n_sp) for i in range(n_sp)]
    down_ring = [(i, (i - 2) % n_sp) for i in range(n_sp)]
    sibling = [(i, i ^ 1) for i in range(n_sp)]
    right = [(i, (i + 1) % n_tp) for i in range(n_tp)]
    left = [(i, (i - 1) % n_tp) for i in range(n_tp)]

    units = mixer_gate.shape[1]
    mixer_rows = jnp.concatenate([mixer_gate, mixer_up, mixer_down.T], axis=1)
    mixer_whole = lax.all_gather(mixer_rows, "sp", axis=0, tiled=True)

    tokens = narrow_query_rows.shape[0]
    narrow_width = narrow_key_value.shape[2] // 2
    wide_width = wide_key_value.shape[2] // 2
    positions = sp_at * tokens + jnp.arange(tokens, dtype=jnp.int32)
    angles_narrow = grid_angles(positions, narrow_width)
    angles_wide = grid_angles(positions, wide_width)
    narrow_keys = prepare(narrow_key_value[:, :, :narrow_width], narrow_norm_gains[1], angles_narrow)
    wide_keys = prepare(wide_key_value[:, :, :wide_width], wide_norm_gains[1], angles_wide)
    own_piece = jnp.concatenate(
        [
            narrow_keys[:, 0],
            narrow_key_value[:, 0, narrow_width:],
            wide_keys[:, 0],
            wide_key_value[:, 0, wide_width:],
        ],
        axis=1,
    )

    narrow_count = narrow_query_rows.shape[1] // narrow_width
    wide_count = wide_query_rows.shape[1] // wide_width
    scales = (LOG2E / math.sqrt(narrow_width), LOG2E / math.sqrt(wide_width))
    widths = [narrow_width] * narrow_count + [wide_width] * wide_count

    hop_up = lax.ppermute(own_piece, "sp", up_ring)
    hop_down = lax.ppermute(own_piece, "sp", down_ring)
    queries = jnp.concatenate(
        [
            head_rows(narrow_query_rows, narrow_norm_gains[0], angles_narrow, narrow_width),
            head_rows(wide_query_rows, wide_norm_gains[0], angles_wide, wide_width),
        ],
        axis=0,
    )
    both = (queries, lax.ppermute(queries, "sp", sibling))

    early = jnp.concatenate([out_narrow, out_wide, residual_in], axis=0)
    early_right = lax.ppermute(early, "tp", right)
    early_left = lax.ppermute(early, "tp", left)

    state = None
    pieces = [own_piece]
    for hop in range(1, chips // 2 + 1):
        pieces += [hop_up, hop_down]
        if state is not None:
            hop_up, hop_down, *state = lax.optimization_barrier((hop_up, hop_down, *state))
        if hop + 1 < chips // 2:
            sent_up, sent_down = (hop_up, hop_down)
        elif hop + 1 == chips // 2:
            sent_up, sent_down = (hop_up[: tokens // 2], hop_down[tokens // 2 :])
        if hop < chips // 2:
            hop_up = lax.ppermute(sent_up, "sp", up_ring)
            hop_down = lax.ppermute(sent_down, "sp", down_ring)
        state = stage(both, pieces, state, narrow_count, narrow_count + wide_count, scales, tokens)
        pieces = []
        if hop == max(chips // 2 - 2, 1):
            narrow_rows = out_narrow.shape[0]
            early_right, early_left, *state = lax.optimization_barrier(
                (early_right, early_left, *state)
            )
            far_narrow = lax.ppermute(early_right[:narrow_rows], "tp", right)
            far_wide = lax.ppermute(early_left[narrow_rows:], "tp", left)

    count = narrow_count + wide_count
    other_acc = lax.ppermute(state[1], "sp", sibling)
    stats = [state[at].reshape(count, tokens, LANES)[:, :, 0].T for at in (3, 5)]
    other_stats = lax.ppermute(jnp.stack(stats), "sp", sibling)
    own = (state[0], state[2], state[4])
    attn = merge(own, (other_acc, other_stats[0], other_stats[1]), widths, tokens)

    cut = narrow_count * narrow_width
    attn_right = lax.ppermute(attn, "tp", right)
    attn_left = lax.ppermute(attn, "tp", left)
    attn_far = (
        lax.ppermute(attn_right[:, :cut], "tp", right),
        lax.ppermute(attn_left[:, cut:], "tp", left),
    )

    normed, own_stream = project(
        tp_at,
        mixer_gain,
        (attn, attn_right, attn_left, *attn_far),
        (out_narrow, out_wide, early_right, early_left, far_narrow, far_wide),
        residual_in,
        cut,
    )
    own, next_up, across, next_down = mix(normed, mixer_whole, units, n_tp)
    far = [(i, (i + 2) % n_tp) for i in range(n_tp)]
    across = lax.ppermute(across, "tp", far)
    next_up = lax.ppermute(next_up, "tp", right)
    next_down = lax.ppermute(next_down, "tp", left)
    parts = [t.astype(jnp.float32) for t in (own, next_up, across, next_down)]
    branch = (parts[0] + parts[1] + parts[2] + parts[3]).astype(jnp.bfloat16)
    return (own_stream + branch.astype(jnp.float32)).astype(jnp.bfloat16)


def solution(mesh):
    placed = (
        P(("grp", "sp", "tp"), None),
        P(("grp", "sp"), "tp"),
        P(("grp", "sp"), "tp"),
        P(("grp", "sp"), "tp", None),
        P(("grp", "sp"), "tp", None),
        P(),
        P(),
        P("tp", None),
        P("tp", None),
        P(),
        P("sp", "tp"),
        P("sp", "tp"),
        P("tp", "sp"),
    )
    return jax.shard_map(
        layer, mesh=mesh, in_specs=placed, out_specs=P(("grp", "sp", "tp"), None), check_vma=False
    )
```

```python
import functools
import math

import jax
import jax.numpy as jnp
from jax import lax
from jax.experimental import pallas as pl
from jax.experimental.pallas import tpu as pltpu
from jax.sharding import PartitionSpec as P


GRID = 64
LANES = 128
LOG2E = math.log2(math.e)

eps = 1e-06
theta = 10000.0


def grid_angles(positions, width):
    quarter = width // 4
    freqs = theta ** (-jnp.arange(quarter, dtype=jnp.float32) * 4.0 / width)
    row = (positions // GRID).astype(jnp.float32)
    column = (positions % GRID).astype(jnp.float32)
    return jnp.concatenate(
        [row[:, None] * freqs[None, :], column[:, None] * freqs[None, :]], axis=-1
    )


def prepare(raw, gain, angles):
    field = raw.astype(jnp.float32)
    field = field * lax.rsqrt(jnp.mean(field * field, axis=-1, keepdims=True) + eps) * gain
    half = field.shape[-1] // 2
    cosine = jnp.cos(angles)[:, None, :]
    sine = jnp.sin(angles)[:, None, :]
    first = field[..., :half]
    second = field[..., half:]
    turned = jnp.concatenate(
        [first * cosine - second * sine, second * cosine + first * sine], axis=-1
    )
    return turned.astype(jnp.bfloat16)


def head_rows(raw, gain, angles, width):
    tokens = raw.shape[0]
    heads = raw.shape[1] // width
    queries = prepare(raw.reshape(tokens, heads, width), gain, angles)
    queries = jnp.transpose(queries, (1, 0, 2)).reshape(heads * tokens, width)
    return jnp.pad(queries, ((0, 0), (0, LANES - width)))


def stage_kernel(*refs, chunks, first, last, split, count, scales, tokens):
    q_refs = refs[:2]
    kv_refs = refs[2 : 2 + chunks]
    refs = refs[2 + chunks :]
    in_refs, out_refs = (None, refs) if first else (refs[:6], refs[6:])
    keys_here = sum(r.shape[0] for r in kv_refs)
    ones = jnp.ones((keys_here, LANES), jnp.bfloat16)

    block = tokens // 2
    low = lax.broadcasted_iota(jnp.int32, (block, LANES), 1) < LANES // 2

    def visit(at, carry):
        narrow = at < 2 * split
        key_at = pl.multiple_of(jnp.where(narrow, 0, LANES), LANES)
        value_at = pl.multiple_of(jnp.where(narrow, 0, 2 * LANES), LANES)
        scale = jnp.where(narrow, scales[0], scales[1])
        rows = pl.ds(pl.multiple_of(at * block, 16), block)
        keys = jnp.concatenate([r[:, pl.ds(key_at, LANES)] for r in kv_refs], axis=0)
        values = jnp.concatenate([r[:, pl.ds(value_at, LANES)] for r in kv_refs], axis=0)
        values = jnp.concatenate([values, ones], axis=1)
        scores = [
            lax.dot_general(
                q[rows, :], keys, (((1,), (1,)), ((), ())), preferred_element_type=jnp.float32
            )
            * scale
            for q in q_refs
        ]
        for side in range(2):
            s = scores[side]
            peak = jnp.max(s, axis=-1, keepdims=True)
            peak = jnp.broadcast_to(peak, (block, LANES))
            if not first:
                old = in_refs[2 + side][rows, :]
                peak = jnp.maximum(peak, old)
                rescale = jnp.exp2(old - peak)
            weights = jnp.concatenate(
                [
                    jnp.exp2(s[:, k : k + LANES] - peak[:, : min(LANES, keys_here - k)])
                    for k in range(0, keys_here, LANES)
                ],
                axis=1,
            ).astype(jnp.bfloat16)
            both = jnp.dot(weights, values, preferred_element_type=jnp.float32)
            summed = both[:, :LANES]
            total = both[:, LANES:]
            if not first:
                total = total + rescale * in_refs[4 + side][rows, :]
                summed = summed + rescale * in_refs[side][rows, :]
            out_refs[side][rows, :] = summed
            if last and side == 1:
                out_refs[3][rows, :] = jnp.where(low, peak, total)
            else:
                out_refs[2 + side][rows, :] = peak
                out_refs[4 + side][rows, :] = total
        return carry

    lax.fori_loop(0, 2 * count, visit, 0)


def stage(queries, pieces, state, last, split, count, scales, tokens):
    rows = queries[0].shape[0]
    keys = sum(p.shape[0] for p in pieces)
    first = state is None
    operands = (*queries, *pieces, *(() if first else state))
    whole = pl.BlockSpec(memory_space=pltpu.VMEM)
    return pl.pallas_call(
        functools.partial(
            stage_kernel,
            chunks=len(pieces),
            first=first,
            last=last,
            split=split,
            count=count,
            scales=scales,
            tokens=tokens,
        ),
        in_specs=[whole] * len(operands),
        out_specs=[whole] * (5 if last else 6),
        out_shape=[jax.ShapeDtypeStruct((rows, LANES), jnp.float32)] * (5 if last else 6),
        compiler_params=pltpu.CompilerParams(vmem_limit_bytes=32 << 20),
        cost_estimate=pl.CostEstimate(
            flops=2 * rows * keys * LANES * 4,
            bytes_accessed=keys * 768 + 12 * rows * LANES * 4,
            transcendentals=2 * rows * keys,
        ),
        name="attend_stage",
    )(*operands)


def merge_kernel(acc_a, peak_a, total_a, acc_b, stats_b, out_ref, *, widths, tokens):
    column = 0
    held = None
    half = LANES // 2
    for h in range(len(widths)):
        rows = slice(h * tokens, (h + 1) * tokens)
        high_a = peak_a[rows, :]
        high_b = stats_b[rows, :1]
        peak = jnp.maximum(high_a, high_b)
        scale_a = jnp.exp2(high_a - peak)
        scale_b = jnp.exp2(high_b - peak)
        total = scale_a * total_a[rows, :] + scale_b * stats_b[rows, half : half + 1]
        summed = scale_a * acc_a[rows, :] + scale_b * acc_b[rows, :]
        result = summed / total
        if widths[h] == LANES:
            out_ref[:, column : column + LANES] = result.astype(out_ref.dtype)
            column += LANES
        elif held is None:
            held = result[:, half:]
        else:
            pair = jnp.concatenate([held, result[:, half:]], axis=1)
            out_ref[:, column : column + LANES] = pair.astype(out_ref.dtype)
            column += LANES
            held = None


def merge(own, other, widths, tokens):
    columns = sum(widths)
    whole = pl.BlockSpec(memory_space=pltpu.VMEM)
    return pl.pallas_call(
        functools.partial(merge_kernel, widths=widths, tokens=tokens),
        in_specs=[whole] * 5,
        out_specs=whole,
        out_shape=jax.ShapeDtypeStruct((tokens, columns), jnp.bfloat16),
        compiler_params=pltpu.CompilerParams(vmem_limit_bytes=32 << 20),
        cost_estimate=pl.CostEstimate(
            flops=8 * len(widths) * tokens * LANES,
            bytes_accessed=16 * len(widths) * tokens * LANES,
            transcendentals=2 * len(widths) * tokens,
        ),
        name="merge_cores",
    )(*own, *other)


def project_kernel(
    at_ref, gain_ref, *refs, split, owned, members
):
    own, right, left, far_narrow, far_wide = refs[:5]
    out_narrow, out_wide, early_right, early_left, early_narrow, early_wide, kept = refs[5:12]
    normed_ref, stream_ref, attended_ref = refs[12:]
    width = attended_ref.shape[1]
    rows = out_narrow.shape[0]
    ends = 2 * rows
    pieces = [
        (own[:, :split], own[:, split:], out_narrow, 0, out_wide, 0),
        (right[:, :split], right[:, split:], early_right, 0, early_right, rows),
        (left[:, :split], left[:, split:], early_left, 0, early_left, rows),
        (far_narrow[...], far_wide[...], early_narrow, 0, early_wide, 0),
    ]
    residuals = [
        kept[...],
        early_left[ends:, :],
        early_wide[rows:, :],
        early_right[ends:, :],
    ]
    block = min(width, 512)

    def visit(at, carry):
        columns = pl.ds(pl.multiple_of(at * block, LANES), block)
        attended = None
        for narrow, wide, first, first_at, second, second_at in pieces:
            part = jnp.dot(
                narrow,
                first[first_at : first_at + rows, columns],
                preferred_element_type=jnp.float32,
            ) + jnp.dot(
                wide,
                second[second_at : second_at + rows, columns],
                preferred_element_type=jnp.float32,
            )
            part = part.astype(jnp.bfloat16).astype(jnp.float32)
            attended = part if attended is None else attended + part
        attended_ref[:, columns] = attended.astype(jnp.bfloat16).astype(jnp.float32)
        return carry

    lax.fori_loop(0, width // block, visit, 0)
    here = at_ref[0]
    for k in range(members):
        start = pl.multiple_of(lax.rem(here + k, members) * owned, 8)
        stream = residuals[k].astype(jnp.float32) + attended_ref[pl.ds(start, owned), :]
        if k == 0:
            stream_ref[...] = stream
        scale = lax.rsqrt(jnp.mean(stream * stream, axis=-1, keepdims=True) + eps)
        normed = stream * scale * gain_ref[...]
        normed_ref[k * owned : (k + 1) * owned, :] = normed.astype(jnp.bfloat16)


def project(at, gain, attn, weights, residual, split):
    owned, width = residual.shape
    rows = attn[0].shape[0]
    operands = (*attn, *weights, residual)
    whole = pl.BlockSpec(memory_space=pltpu.VMEM)
    return pl.pallas_call(
        functools.partial(project_kernel, split=split, owned=owned, members=rows // owned),
        in_specs=[pl.BlockSpec(memory_space=pltpu.SMEM)] + [whole] * (1 + len(operands)),
        out_specs=[whole] * 2,
        out_shape=[
            jax.ShapeDtypeStruct((rows, width), jnp.bfloat16),
            jax.ShapeDtypeStruct((owned, width), jnp.float32),
        ],
        scratch_shapes=[pltpu.VMEM((rows, width), jnp.float32)],
        compiler_params=pltpu.CompilerParams(vmem_limit_bytes=40 << 20),
        cost_estimate=pl.CostEstimate(
            flops=2 * rows * width * 8 * weights[0].shape[0],
            bytes_accessed=16 * width * weights[0].shape[0] + 6 * rows * width,
            transcendentals=rows,
        ),
        name="project",
    )(at.reshape(1), gain.reshape(1, width), *operands)


def mixer_kernel(rows_ref, in_ref, down_ref, *refs):
    out_refs = refs[:-2]
    gate_ref, hidden_ref = refs[-2:]
    step = pl.program_id(0)
    owned = out_refs[0].shape[0]

    @pl.when(step < 2)
    def _():
        product = jnp.dot(rows_ref[...], in_ref[...], preferred_element_type=jnp.float32)

        @pl.when(step == 0)
        def _():
            gate_ref[...] = product

        @pl.when(step == 1)
        def _():
            gate = gate_ref[...]
            hidden = gate / (1.0 + jnp.exp(-gate)) * product
            hidden_ref[...] = hidden.astype(jnp.bfloat16)

    @pl.when(step >= 2)
    def _():
        terms = lax.dot_general(
            hidden_ref[...],
            down_ref[...],
            (((1,), (1,)), ((), ())),
            preferred_element_type=jnp.float32,
        ).astype(jnp.bfloat16)
        for n, out_ref in enumerate(out_refs):
            out_ref[...] = terms[n * owned : (n + 1) * owned, :]


def mix(rows, whole, units, members):
    count, width = rows.shape
    owned = count // members
    depth = min(width, 512)
    return pl.pallas_call(
        mixer_kernel,
        grid=(2 + width // depth,),
        in_specs=[
            pl.BlockSpec((count, width), lambda i: (0, 0)),
            pl.BlockSpec((width, units), lambda i: (0, jnp.minimum(i, 1))),
            pl.BlockSpec((depth, units), lambda i: (jnp.maximum(i - 2, 0), 2)),
        ],
        out_specs=[pl.BlockSpec((owned, depth), lambda i: (0, jnp.maximum(i - 2, 0)))]
        * members,
        out_shape=[jax.ShapeDtypeStruct((owned, width), jnp.bfloat16)] * members,
        scratch_shapes=[
            pltpu.VMEM((count, units), jnp.float32),
            pltpu.VMEM((count, units), jnp.bfloat16),
        ],
        compiler_params=pltpu.CompilerParams(
            vmem_limit_bytes=40 << 20, dimension_semantics=("arbitrary",)
        ),
        cost_estimate=pl.CostEstimate(
            flops=6 * count * width * units,
            bytes_accessed=6 * width * units + 4 * count * width,
            transcendentals=count * units,
        ),
        name="mixer",
    )(rows, whole, whole)


def layer(
    residual_in,
    narrow_query_rows,
    wide_query_rows,
    narrow_key_value,
    wide_key_value,
    narrow_norm_gains,
    wide_norm_gains,
    out_narrow,
    out_wide,
    mixer_gain,
    mixer_gate,
    mixer_up,
    mixer_down,
):
    n_sp = lax.axis_size("sp")
    n_tp = lax.axis_size("tp")
    sp_at = lax.axis_index("sp")
    tp_at = lax.axis_index("tp")
    chips = n_sp // 2
    up_ring = [(i, (i + 2) % n_sp) for i in range(n_sp)]
    down_ring = [(i, (i - 2) % n_sp) for i in range(n_sp)]
    sibling = [(i, i ^ 1) for i in range(n_sp)]
    right = [(i, (i + 1) % n_tp) for i in range(n_tp)]
    left = [(i, (i - 1) % n_tp) for i in range(n_tp)]

    units = mixer_gate.shape[1]
    mixer_rows = jnp.concatenate([mixer_gate, mixer_up, mixer_down.T], axis=1)
    mixer_whole = lax.all_gather(mixer_rows, "sp", axis=0, tiled=True)

    tokens = narrow_query_rows.shape[0]
    narrow_width = narrow_key_value.shape[2] // 2
    wide_width = wide_key_value.shape[2] // 2
    positions = sp_at * tokens + jnp.arange(tokens, dtype=jnp.int32)
    angles_narrow = grid_angles(positions, narrow_width)
    angles_wide = grid_angles(positions, wide_width)
    narrow_keys = prepare(narrow_key_value[:, :, :narrow_width], narrow_norm_gains[1], angles_narrow)
    wide_keys = prepare(wide_key_value[:, :, :wide_width], wide_norm_gains[1], angles_wide)
    own_piece = jnp.concatenate(
        [
            narrow_keys[:, 0],
            narrow_key_value[:, 0, narrow_width:],
            wide_keys[:, 0],
            wide_key_value[:, 0, wide_width:],
        ],
        axis=1,
    )

    narrow_count = narrow_query_rows.shape[1] // narrow_width
    wide_count = wide_query_rows.shape[1] // wide_width
    scales = (LOG2E / math.sqrt(narrow_width), LOG2E / math.sqrt(wide_width))
    widths = [narrow_width] * narrow_count + [wide_width] * wide_count

    hop_up = lax.ppermute(own_piece, "sp", up_ring)
    hop_down = lax.ppermute(own_piece, "sp", down_ring)
    queries = jnp.concatenate(
        [
            head_rows(narrow_query_rows, narrow_norm_gains[0], angles_narrow, narrow_width),
            head_rows(wide_query_rows, wide_norm_gains[0], angles_wide, wide_width),
        ],
        axis=0,
    )
    both = (queries, lax.ppermute(queries, "sp", sibling))

    early = jnp.concatenate([out_narrow, out_wide, residual_in], axis=0)
    early_right = lax.ppermute(early, "tp", right)
    early_left = lax.ppermute(early, "tp", left)

    state = None
    pieces = [own_piece]
    for hop in range(1, chips // 2 + 1):
        pieces += [hop_up, hop_down]
        if state is not None and hop > 2:
            hop_up, hop_down, *state = lax.optimization_barrier((hop_up, hop_down, *state))
        if hop + 1 < chips // 2:
            sent_up, sent_down = (hop_up, hop_down)
        elif hop + 1 == chips // 2:
            sent_up, sent_down = (hop_up[: tokens // 2], hop_down[tokens // 2 :])
        if hop < chips // 2:
            hop_up = lax.ppermute(sent_up, "sp", up_ring)
            hop_down = lax.ppermute(sent_down, "sp", down_ring)
        final = hop == chips // 2
        state = stage(both, pieces, state, final, narrow_count, narrow_count + wide_count, scales, tokens)
        pieces = []
        if hop == max(chips // 2 - 2, 1):
            narrow_rows = out_narrow.shape[0]
            early_right, early_left, *state = lax.optimization_barrier(
                (early_right, early_left, *state)
            )
            far_narrow = lax.ppermute(early_right[:narrow_rows], "tp", right)
            far_wide = lax.ppermute(early_left[narrow_rows:], "tp", left)

    other_acc = lax.ppermute(state[1], "sp", sibling)
    other_stats = lax.ppermute(state[3], "sp", sibling)
    own = (state[0], state[2], state[4])
    attn = merge(own, (other_acc, other_stats), widths, tokens)

    cut = narrow_count * narrow_width
    attn_right = lax.ppermute(attn, "tp", right)
    attn_left = lax.ppermute(attn, "tp", left)
    attn_far = (
        lax.ppermute(attn_right[:, :cut], "tp", right),
        lax.ppermute(attn_left[:, cut:], "tp", left),
    )

    normed, own_stream = project(
        tp_at,
        mixer_gain,
        (attn, attn_right, attn_left, *attn_far),
        (out_narrow, out_wide, early_right, early_left, far_narrow, far_wide),
        residual_in,
        cut,
    )
    own, next_up, across, next_down = mix(normed, mixer_whole, units, n_tp)
    far = [(i, (i + 2) % n_tp) for i in range(n_tp)]
    across = lax.ppermute(across, "tp", far)
    next_up = lax.ppermute(next_up, "tp", right)
    next_down = lax.ppermute(next_down, "tp", left)
    parts = [t.astype(jnp.float32) for t in (own, next_up, across, next_down)]
    branch = (parts[0] + parts[1] + parts[2] + parts[3]).astype(jnp.bfloat16)
    return (own_stream + branch.astype(jnp.float32)).astype(jnp.bfloat16)


def solution(mesh):
    placed = (
        P(("grp", "sp", "tp"), None),
        P(("grp", "sp"), "tp"),
        P(("grp", "sp"), "tp"),
        P(("grp", "sp"), "tp", None),
        P(("grp", "sp"), "tp", None),
        P(),
        P(),
        P("tp", None),
        P("tp", None),
        P(),
        P("sp", "tp"),
        P("sp", "tp"),
        P("tp", "sp"),
    )
    return jax.shard_map(
        layer, mesh=mesh, in_specs=placed, out_specs=P(("grp", "sp", "tp"), None), check_vma=False
    )
```
